32 devices in a mesh: sp: 8 (over z, x), tp: 4 (over y, core).
Axes of the slice: x: 2, y: 2, z: 4, core: 2. Of those that a mesh axis runs over, the one named last changes fastest.
Arguments:
- latent: bfloat16 [9216, 2048], P(('sp', 'tp')), may hold values from -0.6 to 0.6
- context: bfloat16 [32, 2048], P(('sp', 'tp')), may hold values from -6 to 6
- condition: float32 [2048], P('sp'), may hold values from -6 to 6
- context_condition: float32 [2048], P('sp'), may hold values from -6 to 6
- modulation_weight: bfloat16 [2048, 6144], P('sp', 'tp'), may hold values from -0.1875 to 0.1875
- norm_gain: float32 [2048], replicated, may hold values from 0.1 to 1.9
- query_weight: bfloat16 [2048, 1024], replicated
- key_weight: bfloat16 [2048, 256], replicated
- value_weight: bfloat16 [2048, 256], replicated, may hold values from -0.125 to 0.125
- output_weight: bfloat16 [1024, 2048], replicated, may hold values from -0.1875 to 0.1875
- query_gain: float32 [128], replicated, may hold values from 0.5 to 6
- key_gain: float32 [128], replicated, may hold values from 0.5 to 6
- sink_logit: float32 [8], replicated, may hold values from 1 to 5
Outputs:
- updated: bfloat16 [9216, 2048], P(('sp', 'tp'))
The draws below stay inside these ranges and needn't reach their ends.
All inputs are finite; a program needn't handle non-finite values.
Results may differ from the reference program's by a relative error of at most 0.006.
The reference program's roundings to bfloat16 on the way count: a program that leaves them out, or rounds other values in their place, can miss the bound.
Values may be sent and summed in bfloat16 or wider, within the bound.
A program may use at most 64 MiB of HBM per device.

```python
import jax
import jax.numpy as jnp
from jax import lax

D = 2048
HEADS = 8
KV_HEADS = 2
HEAD = 128
WINDOW = 128
GRID_W = 64
TOK_DEV = 288
TOKENS = 9216
CONTEXT = 32


def draw_latent(key, part):
    normal_rows = jnp.clip(jax.random.normal(jax.random.fold_in(key, 1), (TOKENS, D), jnp.float32), -6.0, 6.0)
    return (0.1 * normal_rows).astype(jnp.bfloat16)


def shared_keys(key):
    drawn = jax.random.normal(jax.random.fold_in(key, 21), (D, KV_HEADS * HEAD), jnp.float32)
    return jnp.clip(drawn, -4.0, 4.0) * D ** (-0.5)


def draw_key_weight(key, part):
    return shared_keys(key).astype(jnp.bfloat16)


def draw_query_weight(key, part):
    drawn = jax.random.normal(jax.random.fold_in(key, 22), (D, HEADS * HEAD), jnp.float32)
    drawn = jnp.clip(drawn, -4.0, 4.0) * D ** (-0.5)
    return drawn.astype(jnp.bfloat16)


def draw_query_gain(key, part):
    return jax.random.uniform(jax.random.fold_in(key, 32), (HEAD,), jnp.float32, 0.5, 1.6)


def draw_key_gain(key, part):
    return jax.random.uniform(jax.random.fold_in(key, 34), (HEAD,), jnp.float32, 0.5, 1.6)


def steps_of(rng, shape, pieces, smallest, largest):
    factor_of, own = 1.0, jax.random.fold_in(rng, 6)
    for axis_at, blocks in pieces:
        heights = jnp.exp(jax.random.uniform(jax.random.fold_in(own, axis_at), (blocks,), jnp.float32, smallest / len(pieces), largest / len(pieces)))
        factor_of = factor_of * jnp.repeat(heights, shape[axis_at] // blocks).reshape([-1 if axis == axis_at else 1 for axis in range(len(shape))])
    return factor_of


def bell_draw(key, shape, deviation, bound, cuts=(), kind=jnp.bfloat16):
    entries = jax.random.normal(key, shape, jnp.float32) * deviation
    if len(cuts) > 0:
        entries = steps_of(key, shape, cuts, -0.22, 0.18) * entries
    return jnp.clip(entries, min=-bound, max=bound).astype(kind)


def setup_inputs(seed: int = 0) -> dict:
    key_of = jax.random.split(jax.random.key(seed), 14)
    latent = draw_latent(jax.random.fold_in(key_of[13], 71), 0)
    context = bell_draw(key_of[1], (CONTEXT, D), 1.0, 6.0, ((0, 32),))
    condition = bell_draw(key_of[2], (D,), 1.0, 6.0, ((0, 8),), jnp.float32)
    context_condition = bell_draw(key_of[3], (D,), 1.0, 6.0, ((0, 8),), jnp.float32)
    modulation_weight = bell_draw(key_of[4], (D, 3 * D), (D // 2) ** -0.5, 0.1875, ((0, 8), (1, 4)))
    norm_gain = jnp.clip(1.0 + 0.18 * jax.random.normal(key_of[5], (D,), jnp.float32), 0.1, 1.9)
    query_weight = draw_query_weight(jax.random.fold_in(key_of[13], 71), 0)
    key_weight = draw_key_weight(jax.random.fold_in(key_of[13], 71), 0)
    value_weight = bell_draw(key_of[8], (D, KV_HEADS * HEAD), D ** -0.5, 0.125)
    output_weight = bell_draw(key_of[9], (HEADS * HEAD, D), (HEADS * HEAD) ** -0.5, 0.1875)
    query_gain = draw_query_gain(jax.random.fold_in(key_of[13], 71), 0)
    key_gain = draw_key_gain(jax.random.fold_in(key_of[13], 71), 0)
    sink_logit = jnp.clip(jax.random.uniform(key_of[12], (HEADS,), jnp.float32, 1.0, 5.0), 1.0, 5.0)
    return dict(latent=latent, context=context, condition=condition, context_condition=context_condition, modulation_weight=modulation_weight, norm_gain=norm_gain, query_weight=query_weight, key_weight=key_weight, value_weight=value_weight, output_weight=output_weight, query_gain=query_gain, key_gain=key_gain, sink_logit=sink_logit)


EPS = 1e-06
ROPE_BASE = 10000.0
FAR_LOGIT = -1e+30

def rms_rows(values_in):
    return values_in * lax.rsqrt(lax.optimization_barrier(jnp.mean(values_in * values_in, axis=-1, keepdims=True)) + EPS)

def turn_halves(halves_in):
    former, latter = jnp.split(halves_in, 2, axis=-1)
    return jnp.concatenate([-latter, former], axis=-1)

def rotary(values_in, positions):
    quarter = values_in.shape[-1] // 4
    inverse = jnp.power(ROPE_BASE, -jnp.arange(quarter, dtype=jnp.float32) / quarter)
    by_rows = (positions // GRID_W).astype(jnp.float32)[:, None] * inverse
    by_cols = (positions % GRID_W).astype(jnp.float32)[:, None] * inverse
    angles = jnp.concatenate([by_rows, by_rows, by_cols, by_cols], axis=-1)[:, None, :]
    row_half, col_half = jnp.split(values_in, 2, axis=-1)
    turned = jnp.concatenate([turn_halves(row_half), turn_halves(col_half)], axis=-1)
    return values_in * jnp.cos(angles) + turned * jnp.sin(angles)

def head_norm(flat, gain):
    per_head = flat.reshape(flat.shape[0], flat.shape[1] // gain.shape[0], gain.shape[0])
    return rms_rows(per_head) * gain

def modulated(tokens_in, norm_gain, shift, scale):
    values_in = tokens_in.astype(jnp.float32)
    return (rms_rows(values_in) * norm_gain * (1.0 + scale) + shift).astype(jnp.bfloat16)

def project_ctx(ctx_hidden, key_weight, value_weight, key_gain):
    row_count = ctx_hidden.shape[0]
    ctx_keys = head_norm(jnp.dot(ctx_hidden, key_weight, preferred_element_type=jnp.float32), key_gain)
    ctx_keys = ctx_keys.astype(jnp.bfloat16).reshape(row_count, -1)
    ctx_values = jnp.dot(ctx_hidden, value_weight, preferred_element_type=jnp.float32).astype(jnp.bfloat16)
    return (ctx_keys, ctx_values)

def attend(queries, keys, values, ctx_keys, ctx_values, sink_logit, allowed, head_size):
    row_count = queries.shape[0]
    kv_count = keys.shape[1] // head_size
    group = queries.shape[1] // keys.shape[1]
    score_scale = head_size ** (-0.5)
    grouped = queries.astype(jnp.float32).reshape(row_count, kv_count, group, head_size)
    near_keys = keys.astype(jnp.float32).reshape(-1, kv_count, head_size)
    near_values = values.astype(jnp.float32).reshape(-1, kv_count, head_size)
    far_keys = ctx_keys.astype(jnp.float32).reshape(-1, kv_count, head_size)
    far_values = ctx_values.astype(jnp.float32).reshape(-1, kv_count, head_size)
    near_scores = jnp.einsum('rhgd,khd->hgrk', grouped, near_keys) * score_scale
    near_scores = jnp.where(allowed, near_scores, FAR_LOGIT)
    ctx_scores = jnp.einsum('rhgd,khd->hgrk', grouped, far_keys) * score_scale
    sink_part = sink_logit.reshape(kv_count, group)[:, :, None, None]
    row_max = jnp.maximum(jnp.maximum(lax.optimization_barrier(jnp.max(near_scores, axis=-1, keepdims=True)), lax.optimization_barrier(jnp.max(ctx_scores, axis=-1, keepdims=True))), sink_part)
    near_exp = jnp.exp(near_scores - row_max)
    ctx_exp = jnp.exp(ctx_scores - row_max)
    denominator = lax.optimization_barrier(jnp.sum(near_exp, axis=-1, keepdims=True)) + lax.optimization_barrier(jnp.sum(ctx_exp, axis=-1, keepdims=True)) + jnp.exp(sink_part - row_max)
    near_probs = (near_exp / denominator).astype(jnp.bfloat16).astype(jnp.float32)
    ctx_probs = (ctx_exp / denominator).astype(jnp.bfloat16).astype(jnp.float32)
    mixed = jnp.einsum('hgrk,khd->rhgd', near_probs, near_values) + jnp.einsum('hgrk,khd->rhgd', ctx_probs, far_values)
    return mixed.astype(jnp.bfloat16).reshape(row_count, -1)

def reference(latent, context, condition, context_condition, modulation_weight, norm_gain, query_weight, key_weight, value_weight, output_weight, query_gain, key_gain, sink_logit):
    model_width = latent.shape[1]
    head_size = query_gain.shape[0]
    activations = jax.nn.silu(jnp.stack([condition, context_condition])).astype(jnp.bfloat16)
    modulation = jnp.dot(activations, modulation_weight, preferred_element_type=jnp.float32)
    hidden = modulated(latent, norm_gain, modulation[0, :model_width], modulation[0, model_width:2 * model_width])
    ctx_hidden = modulated(context, norm_gain, modulation[1, :model_width], modulation[1, model_width:2 * model_width])
    gate = modulation[0, 2 * model_width:]
    positions = jnp.arange(TOKENS, dtype=jnp.int32)
    queries = rotary(head_norm(jnp.dot(hidden, query_weight, preferred_element_type=jnp.float32), query_gain), positions).astype(jnp.bfloat16).reshape(TOKENS, -1)
    keys = rotary(head_norm(jnp.dot(hidden, key_weight, preferred_element_type=jnp.float32), key_gain), positions).astype(jnp.bfloat16).reshape(TOKENS, -1)
    values = jnp.dot(hidden, value_weight, preferred_element_type=jnp.float32).astype(jnp.bfloat16)
    ctx_keys, ctx_values = project_ctx(ctx_hidden, key_weight, value_weight, key_gain)
    padded_keys = jnp.pad(keys, ((WINDOW, WINDOW), (0, 0)))
    padded_values = jnp.pad(values, ((WINDOW, WINDOW), (0, 0)))

    def one_block(block_index):
        first_row = block_index * TOK_DEV
        query_block = lax.dynamic_slice_in_dim(queries, first_row, TOK_DEV, 0)
        key_block = lax.dynamic_slice_in_dim(padded_keys, first_row, TOK_DEV + 2 * WINDOW, 0)
        value_block = lax.dynamic_slice_in_dim(padded_values, first_row, TOK_DEV + 2 * WINDOW, 0)
        latent_block = lax.dynamic_slice_in_dim(latent, first_row, TOK_DEV, 0)
        query_pos = first_row + jnp.arange(TOK_DEV, dtype=jnp.int32)
        key_pos = first_row - WINDOW + jnp.arange(TOK_DEV + 2 * WINDOW, dtype=jnp.int32)
        allowed = (jnp.abs(key_pos[None, :] - query_pos[:, None]) <= WINDOW) & (key_pos[None, :] >= 0) & (key_pos[None, :] < TOKENS)
        mixed = attend(query_block, key_block, value_block, ctx_keys, ctx_values, sink_logit, allowed, head_size)
        update = jnp.dot(mixed, output_weight, preferred_element_type=jnp.float32)
        return (latent_block.astype(jnp.float32) + gate * update).astype(jnp.bfloat16)
    blocks = lax.map(one_block, jnp.arange(TOKENS // TOK_DEV, dtype=jnp.int32))
    return blocks.reshape(TOKENS, model_width)
```

```python
import functools
import math

import jax
import jax.numpy as jnp
from jax import lax
from jax.experimental import pallas as pl
from jax.experimental.pallas import tpu as pltpu
from jax.sharding import PartitionSpec as P

WINDOW = 128
GRID_W = 64


EPS = 1e-06
ROPE_BASE = 10000.0
FAR_LOGIT = -1e30
MESH = pl.DeviceIdType.MESH
F32 = jnp.float32
BF16 = jnp.bfloat16


def block_rows_of(rows, extra):
    sizes = [size for size in range(64, rows + 1, 16) if rows % size == 0]
    return min(sizes, key=lambda size: (-(-(size + extra) // 128), -size)) if sizes else rows


def dot(a, b):
    return jnp.dot(a, b, preferred_element_type=F32)


def kernel(
    n_sp, n_tp,
    latent_h, context_ref, cond_ref, ctx_cond_ref, mw_h, norm_gain_ref,
    wq_h, wk_h, wv_h, wo_h, q_gain_ref, k_gain_ref, sink_ref,
    out_h,
    latent_v, mw_v, wq_v, wk_v, wv_v, wo_v, out_v,
    parts, mod_all, ctx_all, ctx_flat, normed, hidden, ctx_hidden,
    cos_v, sin_v, bias_v, q_v, kv_ext, ctx_kv, mixed_v,
    load_sem, out_sem,
    part_send, part_recv, ctx_send, ctx_recv,
    mod_send, mod_recv, row_send, row_recv, halo_send, halo_recv,
):
    rows, width = latent_v.shape
    cols = mw_v.shape[1]
    head = q_gain_ref.shape[-1]
    kv_width = wk_v.shape[1]
    kv_heads = kv_width // head
    heads = wq_v.shape[1] // head
    group = heads // kv_heads
    own_ctx = context_ref.shape[0]
    n_ctx = ctx_flat.shape[0]
    sp, tp = lax.axis_index("sp"), lax.axis_index("tp")
    me = sp * n_tp + tp
    total = n_sp * n_tp
    before = lax.rem(me + total - 1, total)
    after = lax.rem(me + 1, total)

    def place(flat):
        return {"sp": lax.div(flat, n_tp), "tp": lax.rem(flat, n_tp)}

    loads = [
        pltpu.make_async_copy(src, dst, load_sem.at[i])
        for i, (src, dst) in enumerate(
            [(mw_h, mw_v), (latent_h, latent_v), (wk_h, wk_v), (wv_h, wv_v), (wq_h, wq_v), (wo_h, wo_v)]
        )
    ]
    for load in loads:
        load.start()

    barrier = pltpu.get_barrier_semaphore()
    for d in range(1, n_sp):
        pl.semaphore_signal(barrier, inc=1, device_id={"sp": lax.rem(sp + d, n_sp), "tp": tp}, device_id_type=MESH)
    for d in range(1, n_tp):
        pl.semaphore_signal(barrier, inc=1, device_id={"sp": sp, "tp": lax.rem(tp + d, n_tp)}, device_id_type=MESH)
    pl.semaphore_signal(barrier, inc=1, device_id=place(before), device_id_type=MESH)
    pl.semaphore_signal(barrier, inc=1, device_id=place(after), device_id_type=MESH)

    ctx_rows = context_ref[...].astype(F32)
    for r in range(own_ctx):
        ctx_all[tp, sp * own_ctx + r] = ctx_rows[r : r + 1]
    c0 = cond_ref[...].reshape(1, -1)
    c1 = ctx_cond_ref[...].reshape(1, -1)
    pick = lax.broadcasted_iota(jnp.int32, (8, c0.shape[1]), 0) == 0
    both = jnp.where(pick, c0, c1)
    activations = (both * jax.nn.sigmoid(both)).astype(BF16)
    loads[0].wait()
    parts[sp] = dot(activations, mw_v[...])[0:2]

    pl.semaphore_wait(barrier, n_sp + n_tp)

    part_copies, ctx_copies = [], []
    for d in range(1, n_sp):
        there = {"sp": lax.rem(sp + d, n_sp), "tp": tp}
        copy = pltpu.make_async_remote_copy(
            src_ref=parts.at[sp], dst_ref=parts.at[sp],
            send_sem=part_send.at[d], recv_sem=part_recv.at[d],
            device_id=there, device_id_type=MESH,
        )
        copy.start()
        part_copies.append(copy)
    for d in range(1, n_sp):
        there = {"sp": lax.rem(sp + d, n_sp), "tp": tp}
        mine = ctx_all.at[tp, pl.ds(sp * own_ctx, own_ctx)]
        copy = pltpu.make_async_remote_copy(
            src_ref=mine, dst_ref=mine,
            send_sem=ctx_send.at[d], recv_sem=ctx_recv.at[d],
            device_id=there, device_id_type=MESH,
        )
        copy.start()
        ctx_copies.append(copy)

    first = me * rows
    shift_bits = GRID_W.bit_length() - 1
    lane = lax.broadcasted_iota(jnp.int32, (1, head), 1)
    quarter = head // 4
    inverse = jnp.exp((lane % quarter).astype(F32) * (-math.log(ROPE_BASE) / quarter))
    pos = first + lax.broadcasted_iota(jnp.int32, (rows, head), 0)
    by_row = lax.shift_right_logical(pos, shift_bits).astype(F32)
    by_col = lax.bitwise_and(pos, GRID_W - 1).astype(F32)
    angle = jnp.where(lane < 2 * quarter, by_row, by_col) * inverse
    former = lax.rem(lane, 2 * quarter) < quarter
    cos_v[...] = jnp.cos(angle)
    sin_v[...] = jnp.where(former, -1.0, 1.0) * jnp.sin(angle)

    block = bias_v.shape[1]
    span = block + 2 * WINDOW
    for b in range(rows // block):
        qi = lax.broadcasted_iota(jnp.int32, (block, span + n_ctx), 0)
        kj = lax.broadcasted_iota(jnp.int32, (block, span + n_ctx), 1)
        kp = first + (b * block - WINDOW) + kj
        ok = (kj >= qi) & (kj <= qi + 2 * WINDOW) & (kp >= 0) & (kp < rows * total)
        bias_v[b] = jnp.where(ok | (kj >= span), 0.0, FAR_LOGIT)

    gain = norm_gain_ref[...].reshape(1, -1)
    loads[1].wait()
    step = 32

    def norm_rows(i, carry):
        at = pl.ds(pl.multiple_of(i * step, step), step)
        x = latent_v[at, :].astype(F32)
        normed[at, :] = x * lax.rsqrt(jnp.mean(x * x, axis=-1, keepdims=True) + EPS) * gain
        return carry

    lax.fori_loop(0, rows // step, norm_rows, 0)

    for copy in part_copies:
        copy.wait_recv()
    summed = parts[0]
    for i in range(1, n_sp):
        summed = summed + parts[i]
    mod_all[tp] = summed
    mod_copies, row_copies = [], []
    for d in range(1, n_tp):
        there = {"sp": sp, "tp": lax.rem(tp + d, n_tp)}
        copy = pltpu.make_async_remote_copy(
            src_ref=mod_all.at[tp], dst_ref=mod_all.at[tp],
            send_sem=mod_send.at[d], recv_sem=mod_recv.at[d],
            device_id=there, device_id_type=MESH,
        )
        copy.start()
        mod_copies.append(copy)
    for copy in ctx_copies:
        copy.wait_recv()
    for d in range(1, n_tp):
        there = {"sp": sp, "tp": lax.rem(tp + d, n_tp)}
        copy = pltpu.make_async_remote_copy(
            src_ref=ctx_all.at[tp], dst_ref=ctx_all.at[tp],
            send_sem=row_send.at[d], recv_sem=row_recv.at[d],
            device_id=there, device_id_type=MESH,
        )
        copy.start()
        row_copies.append(copy)
    loads[2].wait()
    loads[3].wait()
    for copy in mod_copies:
        copy.wait_recv()
    modulation = jnp.concatenate([mod_all[t] for t in range(n_tp)], axis=1)
    shift_0 = modulation[0:1, :width]
    scale_0 = 1.0 + modulation[0:1, width : 2 * width]
    gate_0 = modulation[0:1, 2 * width :]
    shift_1 = modulation[1:2, :width]
    scale_1 = 1.0 + modulation[1:2, width : 2 * width]

    def modulate_rows(i, carry):
        at = pl.ds(pl.multiple_of(i * step, step), step)
        hidden[at, :] = (normed[at, :] * scale_0 + shift_0).astype(BF16)
        return carry

    lax.fori_loop(0, rows // step, modulate_rows, 0)

    def head_norm(x, gain_ref):
        scale = lax.rsqrt(jnp.mean(x * x, axis=-1, keepdims=True) + EPS)
        return x * scale * gain_ref[...].reshape(1, -1)

    def rotary(x):
        turned = jnp.where(former, pltpu.roll(x, head - quarter, 1), pltpu.roll(x, quarter, 1))
        return x * cos_v[...] + turned * sin_v[...]

    keys = dot(hidden[...], wk_v[...])
    for g in range(kv_heads):
        at = slice(g * head, (g + 1) * head)
        kv_ext[WINDOW : WINDOW + rows, at] = rotary(head_norm(keys[:, at], k_gain_ref)).astype(BF16)
    kv_ext[WINDOW : WINDOW + rows, kv_width:] = dot(hidden[...], wv_v[...]).astype(BF16)

    halo = [
        pltpu.make_async_remote_copy(
            src_ref=kv_ext.at[pl.ds(WINDOW, WINDOW)], dst_ref=kv_ext.at[pl.ds(WINDOW + rows, WINDOW)],
            send_sem=halo_send.at[0], recv_sem=halo_recv.at[0],
            device_id=place(before), device_id_type=MESH,
        ),
        pltpu.make_async_remote_copy(
            src_ref=kv_ext.at[pl.ds(rows, WINDOW)], dst_ref=kv_ext.at[pl.ds(0, WINDOW)],
            send_sem=halo_send.at[1], recv_sem=halo_recv.at[1],
            device_id=place(after), device_id_type=MESH,
        ),
    ]
    for copy in halo:
        copy.start()

    loads[4].wait()
    pair = 2 * head
    for c in range(heads * head // pair):
        both_heads = dot(hidden[...], wq_v[:, c * pair : (c + 1) * pair])
        for k in range(2):
            q_v[2 * c + k] = rotary(
                head_norm(both_heads[:, k * head : (k + 1) * head], q_gain_ref)
            ).astype(BF16)

    for copy in row_copies:
        copy.wait_recv()
    per = n_ctx // n_tp
    for t in range(n_tp):
        for r in range(per):
            ctx_flat[t * per + r : t * per + r + 1, :] = ctx_all[t, r]
    x = ctx_flat[...]
    x = x * lax.rsqrt(jnp.mean(x * x, axis=-1, keepdims=True) + EPS) * gain
    ctx_hidden[...] = (x * scale_1 + shift_1).astype(BF16)
    keys = dot(ctx_hidden[...], wk_v[...])
    for g in range(kv_heads):
        at = slice(g * head, (g + 1) * head)
        ctx_kv[:, at] = head_norm(keys[:, at], k_gain_ref).astype(BF16)
    ctx_kv[:, kv_width:] = dot(ctx_hidden[...], wv_v[...]).astype(BF16)

    for copy in halo:
        copy.wait_recv()

    score_scale = head ** (-0.5)
    for b in range(rows // block):
        base = b * block
        for g in range(kv_heads):
            k_at = slice(g * head, (g + 1) * head)
            v_at = slice(kv_width + g * head, kv_width + (g + 1) * head)
            k_cat = jnp.concatenate([kv_ext[base : base + span, k_at], ctx_kv[:, k_at]], axis=0)
            v_cat = jnp.concatenate([kv_ext[base : base + span, v_at], ctx_kv[:, v_at]], axis=0)
            stacked = jnp.concatenate(
                [q_v[g * group + h, base : base + block, :] for h in range(group)], axis=0
            )
            scores = lax.dot_general(
                stacked, k_cat, (((1,), (1,)), ((), ())), preferred_element_type=F32
            )
            probs = []
            for h in range(group):
                sink = sink_ref[g * group + h]
                s = scores[h * block : (h + 1) * block] * score_scale + bias_v[b]
                m = jnp.maximum(jnp.max(s, axis=-1, keepdims=True), sink)
                e = jnp.exp(s - m)
                denominator = jnp.sum(e, axis=-1, keepdims=True) + jnp.exp(sink - m)
                probs.append((e * (1.0 / denominator)).astype(BF16))
            mixed = dot(jnp.concatenate(probs, axis=0), v_cat).astype(BF16)
            for h in range(group):
                at = (g * group + h) * head
                mixed_v[base : base + block, at : at + head] = mixed[h * block : (h + 1) * block]

    loads[5].wait()
    chunk = 256
    outs = []
    for c in range(width // chunk):
        at = slice(c * chunk, (c + 1) * chunk)
        update = dot(mixed_v[...], wo_v[:, at])
        out_v[:, at] = (latent_v[:, at].astype(F32) + gate_0[:, at] * update).astype(BF16)
        view = pl.ds(c * chunk, chunk)
        copy = pltpu.make_async_copy(out_v.at[:, view], out_h.at[:, view], out_sem.at[c])
        copy.start()
        outs.append(copy)
    for copy in part_copies + ctx_copies + mod_copies + row_copies + halo:
        copy.wait_send()
    for copy in outs:
        copy.wait()


def local(n_sp, n_tp, *args):
    (latent, context, condition, context_condition, modulation_weight, norm_gain,
     query_weight, key_weight, value_weight, output_weight, query_gain, key_gain, sink_logit) = args
    rows, width = latent.shape
    cols = modulation_weight.shape[1]
    n_ctx = context.shape[0] * n_sp * n_tp
    head = query_gain.shape[0]
    kv_width = key_weight.shape[1]
    q_width = query_weight.shape[1]
    block = block_rows_of(rows, 2 * WINDOW + n_ctx)
    dma = pltpu.SemaphoreType.DMA
    hbm = pl.BlockSpec(memory_space=pl.ANY)
    vmem = pl.BlockSpec(memory_space=pltpu.VMEM)
    smem = pl.BlockSpec(memory_space=pltpu.SMEM)
    return pl.pallas_call(
        functools.partial(kernel, n_sp, n_tp),
        out_shape=jax.ShapeDtypeStruct(latent.shape, latent.dtype),
        in_specs=[hbm, vmem, vmem, vmem, hbm, vmem, hbm, hbm, hbm, hbm, vmem, vmem, smem],
        out_specs=hbm,
        scratch_shapes=[
            pltpu.VMEM(latent.shape, BF16),
            pltpu.VMEM(modulation_weight.shape, BF16),
            pltpu.VMEM(query_weight.shape, BF16),
            pltpu.VMEM(key_weight.shape, BF16),
            pltpu.VMEM(value_weight.shape, BF16),
            pltpu.VMEM(output_weight.shape, BF16),
            pltpu.VMEM(latent.shape, BF16),
            pltpu.VMEM((n_sp, 2, cols), F32),
            pltpu.VMEM((n_tp, 2, cols), F32),
            pltpu.VMEM((n_tp, n_ctx // n_tp, 1, width), F32),
            pltpu.VMEM((n_ctx, width), F32),
            pltpu.VMEM((rows, width), F32),
            pltpu.VMEM((rows, width), BF16),
            pltpu.VMEM((n_ctx, width), BF16),
            pltpu.VMEM((rows, head), F32),
            pltpu.VMEM((rows, head), F32),
            pltpu.VMEM((rows // block, block, block + 2 * WINDOW + n_ctx), F32),
            pltpu.VMEM((q_width // head, rows, head), BF16),
            pltpu.VMEM((rows + 2 * WINDOW, 2 * kv_width), BF16),
            pltpu.VMEM((n_ctx, 2 * kv_width), BF16),
            pltpu.VMEM((rows, q_width), BF16),
            dma((6,)),
            dma((width // 256,)),
            dma((n_sp,)), dma((n_sp,)), dma((n_sp,)), dma((n_sp,)),
            dma((n_tp,)), dma((n_tp,)), dma((n_tp,)), dma((n_tp,)),
            dma((2,)), dma((2,)),
        ],
        compiler_params=pltpu.CompilerParams(
            collective_id=0, has_side_effects=True, vmem_limit_bytes=60 * 1024 * 1024
        ),
        name="band_layer",
    )(*args)


def solution(mesh):
    placed = (
        P(("sp", "tp"), None),
        P(("sp", "tp"), None),
        P("sp"),
        P("sp"),
        P("sp", "tp"),
        P(),
        P(),
        P(),
        P(),
        P(),
        P(),
        P(),
        P(),
    )
    body = functools.partial(local, mesh.shape["sp"], mesh.shape["tp"])
    return jax.shard_map(
        body, mesh=mesh, in_specs=placed, out_specs=P(("sp", "tp"), None), check_vma=False
    )
```
